32 devices in a mesh: grp: 2 (over x), ep: 16 (over z, y, core).
Axes of the slice: x: 2, y: 2, z: 4, core: 2. Of those that a mesh axis runs over, the one named last changes fastest.
Arguments:
- tokens: bfloat16 [4096, 2048], P(('grp', 'ep')), parts along dimension 0, may hold values from -6 to 6
- norm_gain: float32 [2048], replicated, may hold values from 0.1 to 1.9
- expert_ids: int32 [4096, 2], P(('grp', 'ep')), parts along dimension 0, may hold values from 0 to 3, all different within a row; in each aligned block of 128 rows (0 to 127, 128 to 255, ...) at most 128 rows name the same one
- route_weight: float32 [4096, 2], P(('grp', 'ep')), parts along dimension 0, may hold values from 0.1 to 1
- gate_weight: bfloat16 [16, 2048, 512], P('ep'), may hold values from -0.375 to 0.375
- up_weight: bfloat16 [16, 2048, 512], P('ep'), may hold values from -0.375 to 0.375
- down_weight: bfloat16 [16, 512, 2048], P('ep'), may hold values from -0.03125 to 0.03125
Outputs:
- combined: bfloat16 [4096, 2048], P(('grp', 'ep')), parts along dimension 0
The draws below stay inside these ranges and needn't reach their ends.
There are 2 independent parts, one for each index of `grp`. The reference program is written for one: setup_inputs(seed, part) draws one part's arguments, and reference() takes and returns one part's arrays. A program takes and returns all parts, laid end to end along the dimension named above; an argument that names none is the same for every part. Nothing has to cross between parts.
Inputs may be any that keep to these rules, and one draw needn't show every extreme that they name: `expert_ids`: each token names 2 different experts; among the tokens of one device no expert is named more than 128 times, and in every draw some expert is named exactly 128 times by the tokens of some device.
All inputs are finite; a program needn't handle non-finite values.
Results may differ from the reference program's by a relative error of at most 0.0078.
Values may be sent and summed in bfloat16 or wider, within the bound.
A program may use at most 128 MiB of HBM per device.

```python
import math
import jax
import jax.numpy as jnp
import numpy as np
from jax import lax

D = 2048
FF = 2048
SPLIT = 4
FF_DEV = 512
TOP_K = 2
TOK_DEV = 128
EXPERTS = 4
CAP = 128
TOKENS = 2048
N_EP = 16


def levels(stream_key, extent, pieces, low, largest):
    factor_of, own = 1.0, jax.random.fold_in(stream_key, 6)
    for position, shards_of in pieces:
        steps = jnp.exp(jax.random.uniform(jax.random.fold_in(own, position), (shards_of,), jnp.float32, low / len(pieces), largest / len(pieces)))
        factor_of = factor_of * jnp.repeat(steps, extent[position] // shards_of).reshape([-1 if axis == position else 1 for axis in range(len(extent))])
    return factor_of


def assign_block(own_key, own, number, rows, amount, top, bound, skew):
    sequence = jax.random.permutation(own_key, amount)
    crowded, ordinary = shares(amount, rows * top, bound, skew, True), shares(amount, rows * top, bound, skew, False)
    places = jnp.arange(amount)

    def named(tallies, turn):
        used = int((tallies > 0).sum())
        fixed = max(1, used // 4)
        shifted = fixed + (places - fixed + turn * (used - fixed)) % max(1, amount - fixed)
        return jnp.zeros((amount,), jnp.int32).at[sequence[jnp.where(places < fixed, places, shifted)]].set(jnp.asarray(tallies, jnp.int32))

    tallies = jnp.where(number % 4 == 0, named(crowded, number // 4), named(ordinary, number - number // 4 - 1))
    mixed = jax.random.permutation(jax.random.fold_in(own, 3), amount)
    source_of, receiver = mixed[0:amount // 2 * 2:2], mixed[1:amount // 2 * 2:2]
    margin = jnp.minimum(tallies[source_of] - 1, bound - tallies[receiver]) // 2
    margin = jnp.where((source_of == sequence[0]) | (receiver == sequence[0]) | (tallies[receiver] == 0), 0, jnp.maximum(margin, 0))
    shifted = jax.random.randint(jax.random.fold_in(own, 4), (amount // 2,), 0, 1 << 20) % (margin + 1)
    tallies = tallies.at[source_of].add(-shifted).at[receiver].add(shifted)
    items = jnp.searchsorted(jnp.cumsum(tallies), jnp.arange(rows * top), side="right").astype(jnp.int32)
    table = items.reshape(top, rows).T
    table = table[jax.random.permutation(jax.random.fold_in(own, 1), rows)]
    turn = jax.random.randint(jax.random.fold_in(own, 2), (rows, 1), 0, top)
    return jnp.take_along_axis(table, (jnp.arange(top)[None, :] + turn) % top, axis=1)


def shares(amount, total, limit, slope, full):
    loads = [(1 << 20) // math.isqrt(rank ** slope) + 1 for rank in range(1, amount + 1)]
    largest = limit if full else min(limit, max(-(-total // amount), total * loads[0] // sum(loads)))
    least = 1 if total - largest >= amount - 1 else 0
    holding, rest = [largest] + [least] * (amount - 1), total - largest - least * (amount - 1)
    while rest > 0:
        candidates = [i for i in range(1, amount) if holding[i] < largest] or [i for i in range(1, amount) if holding[i] < limit]
        whole, budget = sum([loads[i] for i in candidates]), rest
        for i in candidates:
            extra = min(limit - holding[i], max(1, budget * loads[i] // whole), rest)
            holding[i] = holding[i] + extra
            rest = rest - extra
    return np.array(holding)


def normal_values(stream_key, dims, width, reach, cuts=(), held_as=jnp.bfloat16):
    drawn = width * jax.random.normal(stream_key, dims, jnp.float32)
    if cuts:
        drawn = drawn * levels(stream_key, dims, cuts, -0.22, 0.18)
    return jnp.clip(drawn, -reach, reach).astype(held_as)


def setup_inputs(seed: int = 0, part: int = 0) -> dict:
    key_list = jax.random.split(jax.random.key(seed), 8)
    part_keys = jax.random.split(jax.random.fold_in(key_list[7], part), 8)
    tokens = normal_values(part_keys[0], (TOKENS, D), 1.0, 6.0, ((0, 16),))
    norm_gain = jnp.clip(1.0 + 0.18 * jax.random.normal(key_list[1], (D,), jnp.float32), 0.1, 1.9)
    expert_ids_keys = jax.random.split(jax.random.fold_in(part_keys[2], 1), TOKENS // TOK_DEV)
    expert_ids_turns = jax.random.permutation(jax.random.fold_in(part_keys[2], 3), TOKENS // TOK_DEV)
    expert_ids = jax.vmap(lambda own, number: assign_block(jax.random.fold_in(part_keys[2], 2), own, number, TOK_DEV, EXPERTS, TOP_K, CAP, 2))(expert_ids_keys, expert_ids_turns).reshape((TOKENS, TOP_K))
    route_weight = jnp.clip(jnp.exp(math.log(1.0) - 2.3025851 * jax.random.uniform(part_keys[3], (TOKENS, TOP_K), jnp.float32) ** levels(part_keys[3], (TOKENS, TOP_K), ((0, 16),), -0.2, 0.2)), 0.1, 1.0)
    gate_weight = normal_values(key_list[4], (N_EP, D, FF_DEV), (D // 8) ** -0.5, 0.375, ((0, 16),))
    up_weight = normal_values(key_list[5], (N_EP, D, FF_DEV), (D // 8) ** -0.5, 0.375, ((0, 16),))
    down_weight = normal_values(key_list[6], (N_EP, FF_DEV, D), (16 * FF) ** -0.5, 0.03125, ((0, 16),))
    return dict(tokens=tokens, norm_gain=norm_gain, expert_ids=expert_ids, route_weight=route_weight, gate_weight=gate_weight, up_weight=up_weight, down_weight=down_weight)


EPSILON = 1e-05
clamp_limit = 7.0
sigmoid_slope = 1.702
row_block = 256

def reference(tokens, norm_gain, expert_ids, route_weight, gate_weight, up_weight, down_weight):
    values = tokens.astype(jnp.float32)
    center = values - lax.optimization_barrier(jnp.mean(values, axis=-1, keepdims=True))
    spread = lax.optimization_barrier(jnp.mean(center * center, axis=-1, keepdims=True))
    normed = (center * lax.rsqrt(spread + EPSILON) * norm_gain).astype(jnp.bfloat16)
    w_gate = gate_weight.reshape(EXPERTS, SPLIT, D, FF_DEV).transpose(0, 2, 1, 3).reshape(EXPERTS, D, FF)
    w_up = up_weight.reshape(EXPERTS, SPLIT, D, FF_DEV).transpose(0, 2, 1, 3).reshape(EXPERTS, D, FF)
    w_down = down_weight.reshape(EXPERTS, FF, D)
    assigned = TOKENS * TOP_K
    flat_ids = expert_ids.reshape(assigned).astype(jnp.int32)
    owners = jnp.arange(assigned, dtype=jnp.int32) // TOP_K
    ranking = jnp.argsort(flat_ids, stable=True).astype(jnp.int32)
    sorted_ids = flat_ids[ranking]
    counts = lax.optimization_barrier(jnp.sum((flat_ids[:, None] == jnp.arange(EXPERTS, dtype=jnp.int32)[None, :]).astype(jnp.int32), axis=0))
    starts = jnp.cumsum(counts) - counts
    padded_counts = (counts + row_block - 1) // row_block * row_block
    block_ends = jnp.cumsum(padded_counts)
    begins = block_ends - padded_counts
    target = (begins[sorted_ids] + jnp.arange(assigned, dtype=jnp.int32) - starts[sorted_ids]).astype(jnp.int32)
    blocks = -(-assigned // row_block) + EXPERTS
    slot_token = jnp.full((blocks * row_block,), TOKENS, jnp.int32).at[target].set(owners[ranking])
    first_rows = jnp.arange(blocks, dtype=jnp.int32) * row_block
    block_expert = jnp.minimum(lax.optimization_barrier(jnp.sum((first_rows[:, None] >= block_ends[None, :]).astype(jnp.int32), axis=1)), EXPERTS - 1).astype(jnp.int32)
    padded = jnp.concatenate([normed, jnp.zeros((1, D), jnp.bfloat16)], axis=0)
    gathered_rows = jnp.take(padded, slot_token, axis=0).reshape(blocks, row_block, D)

    def block_fn(operands):
        block_rows, expert = operands
        gate_pre = jnp.dot(block_rows, w_gate[expert], preferred_element_type=jnp.float32)
        up_pre = jnp.dot(block_rows, w_up[expert], preferred_element_type=jnp.float32)
        gate_cut = jnp.minimum(gate_pre, clamp_limit)
        up_cut = jnp.clip(up_pre, -clamp_limit, clamp_limit)
        active = ((up_cut + 1.0) * (gate_cut * jax.nn.sigmoid(gate_cut * sigmoid_slope))).astype(jnp.bfloat16)
        return jnp.dot(active, w_down[expert], preferred_element_type=jnp.float32).astype(jnp.bfloat16)
    outputs = lax.map(block_fn, (gathered_rows, block_expert)).reshape(blocks * row_block, D)
    sorted_out = jnp.take(outputs, target, axis=0)
    picked = jnp.zeros((assigned, D), jnp.bfloat16).at[ranking].set(sorted_out).reshape(TOKENS, TOP_K, D)
    combined = lax.optimization_barrier(jnp.sum(route_weight[:, :, None] * picked.astype(jnp.float32), axis=1))
    return combined.astype(jnp.bfloat16)
```

```python
import functools

import jax
import jax.numpy as jnp
from jax import lax
from jax.experimental import pallas as pl
from jax.experimental.pallas import tpu as pltpu
from jax.sharding import PartitionSpec as P

SPLIT = 4


EPSILON = 1e-05
clamp_limit = 7.0
sigmoid_slope = 1.702


def swapped(array, axis, bit):
    return lax.ppermute(array, axis, [(i, i ^ 1 << bit) for i in range(lax.axis_size(axis))])


def layer_norm(tokens, norm_gain):
    values = tokens.astype(jnp.float32)
    center = values - jnp.mean(values, axis=-1, keepdims=True)
    spread = jnp.mean(center * center, axis=-1, keepdims=True)
    return (center * lax.rsqrt(spread + EPSILON) * norm_gain).astype(jnp.bfloat16)


def expert_rows(block_rows, gate_weight, up_weight, down_weight):
    gate_pre = jnp.einsum(
        "scd,df->scf", block_rows, gate_weight[0], preferred_element_type=jnp.float32
    )
    up_pre = jnp.einsum("scd,df->scf", block_rows, up_weight[0], preferred_element_type=jnp.float32)
    gate_cut = jnp.minimum(gate_pre, clamp_limit)
    up_cut = jnp.clip(up_pre, -clamp_limit, clamp_limit)
    active = ((up_cut + 1.0) * (gate_cut * jax.nn.sigmoid(gate_cut * sigmoid_slope))).astype(
        jnp.bfloat16
    )
    return jnp.einsum("scf,fd->scd", active, down_weight[0], preferred_element_type=jnp.float32)


def slot_body(tokens, norm_gain, expert_ids, route_weight, gate_weight, up_weight, down_weight):
    normed = layer_norm(tokens, norm_gain)
    devices = lax.axis_size("ep")
    experts = devices // SPLIT
    tok_rows = tokens.shape[0]
    top_count = expert_ids.shape[1]
    width = tokens.shape[1]
    capacity = min(tok_rows, 2 * tok_rows * top_count // experts)
    quarter = capacity // SPLIT
    levels = SPLIT.bit_length() - 1
    position = lax.axis_index("ep")
    flat_ids = expert_ids.reshape(-1)
    onehot = (flat_ids[:, None] == jnp.arange(experts, dtype=jnp.int32)[None, :]).astype(jnp.int32)
    earlier = jnp.cumsum(onehot, axis=0) - onehot
    slot_index = jnp.sum(earlier * onehot, axis=1)
    target = flat_ids * capacity + slot_index
    owners = jnp.arange(flat_ids.shape[0], dtype=jnp.int32) // top_count
    slot_token = jnp.full((experts * capacity,), tok_rows, jnp.int32).at[target].set(owners)
    padded = jnp.concatenate([normed, jnp.zeros((1, width), jnp.bfloat16)], axis=0)
    outgoing = jnp.take(padded, slot_token, axis=0).reshape(experts, capacity, width)
    pieces = outgoing.reshape(devices, quarter, width)
    gathered = lax.all_to_all(pieces, "ep", split_axis=0, concat_axis=0, tiled=True)
    for bit_level in range(levels):
        partner = swapped(gathered, "ep", bit_level)
        upper_bit = position >> bit_level & 1
        first_half = jnp.where(upper_bit == 1, partner, gathered)
        second_half = jnp.where(upper_bit == 1, gathered, partner)
        gathered = jnp.concatenate([first_half, second_half], axis=1)
    partial_value = expert_rows(gathered, gate_weight, up_weight, down_weight)
    length = capacity
    for bit_level in reversed(range(levels)):
        length = length // 2
        upper_bit = position >> bit_level & 1
        kept_rows = lax.dynamic_slice_in_dim(partial_value, upper_bit * length, length, 1)
        sent_rows = lax.dynamic_slice_in_dim(partial_value, (1 - upper_bit) * length, length, 1)
        partial_value = kept_rows + swapped(sent_rows, "ep", bit_level)
    finished = partial_value.astype(jnp.bfloat16)
    returned = lax.all_to_all(finished, "ep", split_axis=0, concat_axis=0, tiled=True)
    results = returned.reshape(experts * capacity, width)
    picked = jnp.take(results, target, axis=0).reshape(tok_rows, top_count, width)
    combined = jnp.sum(route_weight[:, :, None] * picked.astype(jnp.float32), axis=1)
    return combined.astype(jnp.bfloat16)


MESH = pl.DeviceIdType.MESH
HALVES = 2


def near_plane(z, k, planes):
    below, above = z, planes - 1 - z
    short = jnp.minimum(below, above)
    side = jnp.where(above >= below, 1, -1)
    paired = jnp.where(k % 2 == 1, side * ((k + 1) // 2), -side * (k // 2))
    return z + jnp.where(k <= 2 * short, paired, side * (k - short))


def lane_to_column(row, rows):
    eye = lax.broadcasted_iota(jnp.int32, (rows, rows), 0) == lax.broadcasted_iota(
        jnp.int32, (rows, rows), 1
    )
    return jnp.sum(jnp.where(eye, row, 0.0), axis=1, keepdims=True)


def column_to_lane(column, rows):
    eye = lax.broadcasted_iota(jnp.int32, (rows, rows), 0) == lax.broadcasted_iota(
        jnp.int32, (rows, rows), 1
    )
    return jnp.sum(jnp.where(eye, column, 0.0), axis=0, keepdims=True)


def dense_kernel(
    devices,
    tokens_ref, gain_ref, ids_ref, route_ref, gate_hbm, up_hbm, down_hbm,
    out_ref,
    tok, part, cbuf, ybuf, zbuf, acc, wsend, wbuf, gate, up, down,
    wsem, gsend, grecv, rsend_c, rrecv_c, rsend_y, rrecv_y, rsend_z, rrecv_z, ssend, srecv,
):
    planes = devices // SPLIT
    rows, width = tokens_ref.shape
    half = rows // HALVES
    me = lax.axis_index("ep")
    z, y, c = me // 4, (me // 2) % 2, me % 2

    def index(zp, yp, cp):
        return zp * 4 + yp * 2 + cp

    ypeer, cpeer = index(z, 1 - y, c), index(z, y, 1 - c)

    def span(h):
        return pl.ds(h * half, half)

    def remote(source, target, send_sem, recv_sem, device):
        return pltpu.make_async_remote_copy(
            src_ref=source, dst_ref=target, send_sem=send_sem, recv_sem=recv_sem,
            device_id={"ep": device}, device_id_type=MESH,
        )

    def move(kind, i, h, device):
        return remote(
            tok.at[i, span(h)], tok.at[i, span(h)], gsend.at[kind, i, h], grecv.at[i, h], device
        )

    weight_loads = [
        pltpu.make_async_copy(gate_hbm.at[0], gate, wsem.at[0]),
        pltpu.make_async_copy(up_hbm.at[0], up, wsem.at[1]),
        pltpu.make_async_copy(down_hbm.at[0], down, wsem.at[2]),
    ]
    for load in weight_loads:
        load.start()

    barrier = pltpu.get_barrier_semaphore()
    for step in range(1, devices):
        pl.semaphore_signal(
            barrier, inc=1, device_id={"ep": (me + step) % devices}, device_id_type=MESH
        )
    for h in range(HALVES):
        values = tokens_ref[span(h), :].astype(jnp.float32)
        center = values - jnp.mean(values, axis=-1, keepdims=True)
        spread = jnp.mean(center * center, axis=-1, keepdims=True)
        tok[me, span(h), :] = (center * lax.rsqrt(spread + EPSILON) * gain_ref[...]).astype(
            jnp.bfloat16
        )
    for e in range(planes):
        column = jnp.sum(jnp.where(ids_ref[...] == e, route_ref[...], 0.0), axis=1, keepdims=True)
        wsend[e] = jnp.broadcast_to(column_to_lane(column, rows), (8, rows))
    pl.semaphore_wait(barrier, devices - 1)

    has_up, has_down = z < planes - 1, z > 0
    for h in range(HALVES):
        move(2, me, h, ypeer).start()
        pl.when(has_up)(lambda: move(0, me, h, me + 4).start())
        pl.when(has_down)(lambda: move(1, me, h, me - 4).start())
        move(3, me, h, cpeer).start()

    def share(step):
        there = (me + step) % devices
        return remote(wsend.at[there // SPLIT], wbuf.at[me], ssend.at[there], srecv.at[me], there)

    def shared(step):
        there = (me + step) % devices
        return remote(wsend.at[z], wbuf.at[there], ssend.at[there], srecv.at[there], there)

    for step in range(1, devices):
        share(step).start()
    wbuf[me] = wsend[z]
    for load in weight_loads:
        load.wait()
    for step in range(1, devices):
        shared(step).wait_recv()

    def onward(zp):
        return jnp.where(zp < z, z + 1, z - 1)

    def exists(plane):
        return jnp.logical_and(plane >= 0, plane < planes)

    def compute(zp, yp):
        first = index(zp, yp, 0)
        x = tok[pl.ds(first, 2)].reshape(2 * rows, width)
        gate_cut = jnp.minimum(
            jnp.dot(x, gate[...], preferred_element_type=jnp.float32), clamp_limit
        )
        up_cut = jnp.clip(
            jnp.dot(x, up[...], preferred_element_type=jnp.float32), -clamp_limit, clamp_limit
        )
        active = ((up_cut + 1.0) * (gate_cut * jax.nn.sigmoid(gate_cut * sigmoid_slope))).astype(
            jnp.bfloat16
        )
        scale = jnp.concatenate(
            [lane_to_column(wbuf[first + lane, 0:1, :], rows) for lane in range(2)], axis=0
        )
        tile = min(512, width)
        for start in range(0, width, tile):
            value = jnp.dot(
                active, down[:, start : start + tile], preferred_element_type=jnp.float32
            )
            part[pl.ds(first, 2), :, start : start + tile] = (
                (value * scale).astype(jnp.bfloat16).reshape(2, rows, tile)
            )

    def to_core(zp, yp):
        group = zp * 2 + yp
        return remote(
            part.at[index(zp, yp, 1 - c)], cbuf.at[group],
            rsend_c.at[group], rrecv_c.at[group], cpeer,
        )

    def gather_step(k, _):
        zk = near_plane(z, jnp.minimum(k, planes - 1), planes)
        zb = near_plane(z, jnp.maximum(k - 1, 0), planes)

        @pl.when(jnp.logical_and(k > 0, k < planes))
        def _():
            i = index(zk, y, c)
            nz = onward(zk)
            for h in range(HALVES):
                move(2, i, h, ypeer).wait_recv()
                pl.when(exists(nz))(lambda: move(0, i, h, index(nz, y, c)).start())
                move(2, i, h, ypeer).start()
                move(3, i, h, cpeer).start()

        @pl.when(k > 0)
        def _():
            i = index(zb, 1 - y, c)
            for h in range(HALVES):
                move(3, i, h, cpeer).wait_recv()
                move(3, i, h, cpeer).start()

        def group_step(j, _):
            zp = jnp.where(j == 0, zk, zb)
            yp = jnp.where(j == 0, y, 1 - y)

            @pl.when(jnp.where(j == 0, planes - k, k) > 0)
            def _():
                for h in range(HALVES):
                    move(3, index(zp, yp, 1 - c), h, cpeer).wait_recv()
                compute(zp, yp)
                to_core(zp, yp).start()

            return 0

        lax.fori_loop(0, 2, group_step, 0)
        return 0

    lax.fori_loop(0, planes + 1, gather_step, 0)

    def to_y(zp, h):
        return remote(
            part.at[index(zp, 1 - y, c), span(h)], ybuf.at[zp, span(h)],
            rsend_y.at[zp, h], rrecv_y.at[zp, h], ypeer,
        )

    def from_y(zp, h):
        return remote(
            part.at[index(zp, y, c), span(h)], ybuf.at[zp, span(h)],
            rsend_y.at[zp, h], rrecv_y.at[zp, h], ypeer,
        )

    def spread_step(t, _):
        zp = near_plane(z, planes - 1 - t, planes)
        to_core(zp, 1 - y).wait_recv()
        i = index(zp, 1 - y, c)
        for h in range(HALVES):
            part[i, span(h), :] = (
                part[i, span(h), :].astype(jnp.float32)
                + cbuf[zp * 2 + 1 - y, span(h), :].astype(jnp.float32)
            ).astype(jnp.bfloat16)
            to_y(zp, h).start()
        return 0

    lax.fori_loop(0, planes, spread_step, 0)

    def hop(zp, h):
        nz = jnp.where(zp > z, z + 1, z - 1)
        slot = jnp.where(jnp.logical_and(nz == zp, zp < z), planes, zp)
        return remote(
            part.at[index(zp, y, c), span(h)], zbuf.at[slot, span(h)],
            rsend_z.at[zp, h], rrecv_z.at[slot, h], index(nz, y, c),
        )

    def landed(slot, h):
        return remote(
            part.at[me, span(h)], zbuf.at[slot, span(h)],
            rsend_z.at[z, h], rrecv_z.at[slot, h], ypeer,
        )

    def add_landed(slot, h):
        landed(slot, h).wait_recv()
        acc[...] += zbuf[slot, span(h), :].astype(jnp.float32)

    def total(zp, h):
        from_y(zp, h).wait_recv()
        acc[...] = (
            part[index(zp, y, c), span(h), :].astype(jnp.float32)
            + cbuf[zp * 2 + y, span(h), :].astype(jnp.float32)
            + ybuf[zp, span(h), :].astype(jnp.float32)
        )

    def chain_step(t, _):
        zp = near_plane(z, planes - 1 - t, planes)
        to_core(zp, y).wait_recv()
        for h in range(HALVES):
            total(zp, h)
            pl.when(jnp.where(zp > z, has_down, has_up))(lambda: add_landed(zp, h))
            part[index(zp, y, c), span(h), :] = acc[...].astype(jnp.bfloat16)
            hop(zp, h).start()
        return 0

    lax.fori_loop(0, planes - 1, chain_step, 0)
    to_core(z, y).wait_recv()
    for h in range(HALVES):
        total(z, h)
        pl.when(has_down)(lambda: add_landed(z, h))
        pl.when(has_up)(lambda: add_landed(planes, h))
        out_ref[span(h), :] = acc[...].astype(jnp.bfloat16)

    for step in range(1, devices):
        share(step).wait_send()
    for h in range(HALVES):
        move(2, me, h, ypeer).wait_send()
        pl.when(has_up)(lambda: move(0, me, h, me + 4).wait_send())
        pl.when(has_down)(lambda: move(1, me, h, me - 4).wait_send())
        move(3, me, h, cpeer).wait_send()

    def drain_step(k, _):
        zp = near_plane(z, k, planes)
        to_core(zp, y).wait_send()
        to_core(zp, 1 - y).wait_send()
        for h in range(HALVES):
            move(3, index(zp, 1 - y, c), h, cpeer).wait_send()
            to_y(zp, h).wait_send()

        @pl.when(k > 0)
        def _():
            i = index(zp, y, c)
            nz = onward(zp)
            for h in range(HALVES):
                pl.when(exists(nz))(lambda: move(0, i, h, index(nz, y, c)).wait_send())
                move(2, i, h, ypeer).wait_send()
                move(3, i, h, cpeer).wait_send()
                hop(zp, h).wait_send()

        return 0

    lax.fori_loop(0, planes, drain_step, 0)


def dense_body(tokens, norm_gain, expert_ids, route_weight, gate_weight, up_weight, down_weight):
    devices = lax.axis_size("ep")
    planes = devices // SPLIT
    rows, width = tokens.shape
    hidden = gate_weight.shape[2]
    half = rows // HALVES
    vmem, dma = pltpu.VMEM, pltpu.SemaphoreType.DMA
    block = jnp.bfloat16
    return pl.pallas_call(
        functools.partial(dense_kernel, devices),
        out_shape=jax.ShapeDtypeStruct((rows, width), block),
        in_specs=[pl.BlockSpec(memory_space=vmem)] * 4 + [pl.BlockSpec(memory_space=pl.ANY)] * 3,
        out_specs=pl.BlockSpec(memory_space=vmem),
        scratch_shapes=[
            vmem((devices, rows, width), block),
            vmem((devices, rows, width), block),
            vmem((2 * planes, rows, width), block),
            vmem((planes, rows, width), block),
            vmem((planes + 1, rows, width), block),
            vmem((half, width), jnp.float32),
            vmem((planes, 8, rows), jnp.float32),
            vmem((devices, 8, rows), jnp.float32),
            vmem((width, hidden), block),
            vmem((width, hidden), block),
            vmem((hidden, width), block),
            dma((3,)),
            dma((4, devices, HALVES)),
            dma((devices, HALVES)),
            dma((2 * planes,)),
            dma((2 * planes,)),
            dma((planes, HALVES)),
            dma((planes, HALVES)),
            dma((planes, HALVES)),
            dma((planes + 1, HALVES)),
            dma((devices,)),
            dma((devices,)),
        ],
        compiler_params=pltpu.CompilerParams(
            collective_id=0, has_side_effects=True, vmem_limit_bytes=60 * 1024 * 1024
        ),
        name="dense_experts",
    )(
        tokens, norm_gain.reshape(1, width), expert_ids, route_weight,
        gate_weight, up_weight, down_weight,
    )


def body(tokens, norm_gain, expert_ids, route_weight, gate_weight, up_weight, down_weight):
    tok_rows, top_count = expert_ids.shape
    experts = lax.axis_size("ep") // SPLIT
    capacity = min(tok_rows, 2 * tok_rows * top_count // experts)
    chosen = dense_body if capacity == tok_rows else slot_body
    return chosen(
        tokens, norm_gain, expert_ids, route_weight, gate_weight, up_weight, down_weight
    )


def solution(mesh):
    placed = (
        P(("grp", "ep"), None),
        P(),
        P(("grp", "ep"), None),
        P(("grp", "ep"), None),
        P("ep", None, None),
        P("ep", None, None),
        P("ep", None, None),
    )
    return jax.shard_map(
        body, mesh=mesh, in_specs=placed, out_specs=P(("grp", "ep"), None), check_vma=False
    )
```

```python
import functools

import jax
import jax.numpy as jnp
from jax import lax
from jax.experimental import pallas as pl
from jax.experimental.pallas import tpu as pltpu
from jax.sharding import PartitionSpec as P

SPLIT = 4


EPSILON = 1e-05
clamp_limit = 7.0
sigmoid_slope = 1.702


def swapped(array, axis, bit):
    return lax.ppermute(array, axis, [(i, i ^ 1 << bit) for i in range(lax.axis_size(axis))])


def layer_norm(tokens, norm_gain):
    values = tokens.astype(jnp.float32)
    center = values - jnp.mean(values, axis=-1, keepdims=True)
    spread = jnp.mean(center * center, axis=-1, keepdims=True)
    return (center * lax.rsqrt(spread + EPSILON) * norm_gain).astype(jnp.bfloat16)


def expert_rows(block_rows, gate_weight, up_weight, down_weight):
    gate_pre = jnp.einsum(
        "scd,df->scf", block_rows, gate_weight[0], preferred_element_type=jnp.float32
    )
    up_pre = jnp.einsum("scd,df->scf", block_rows, up_weight[0], preferred_element_type=jnp.float32)
    gate_cut = jnp.minimum(gate_pre, clamp_limit)
    up_cut = jnp.clip(up_pre, -clamp_limit, clamp_limit)
    active = ((up_cut + 1.0) * (gate_cut * jax.nn.sigmoid(gate_cut * sigmoid_slope))).astype(
        jnp.bfloat16
    )
    return jnp.einsum("scf,fd->scd", active, down_weight[0], preferred_element_type=jnp.float32)


def slot_body(tokens, norm_gain, expert_ids, route_weight, gate_weight, up_weight, down_weight):
    normed = layer_norm(tokens, norm_gain)
    devices = lax.axis_size("ep")
    experts = devices // SPLIT
    tok_rows = tokens.shape[0]
    top_count = expert_ids.shape[1]
    width = tokens.shape[1]
    capacity = min(tok_rows, 2 * tok_rows * top_count // experts)
    quarter = capacity // SPLIT
    levels = SPLIT.bit_length() - 1
    position = lax.axis_index("ep")
    flat_ids = expert_ids.reshape(-1)
    onehot = (flat_ids[:, None] == jnp.arange(experts, dtype=jnp.int32)[None, :]).astype(jnp.int32)
    earlier = jnp.cumsum(onehot, axis=0) - onehot
    slot_index = jnp.sum(earlier * onehot, axis=1)
    target = flat_ids * capacity + slot_index
    owners = jnp.arange(flat_ids.shape[0], dtype=jnp.int32) // top_count
    slot_token = jnp.full((experts * capacity,), tok_rows, jnp.int32).at[target].set(owners)
    padded = jnp.concatenate([normed, jnp.zeros((1, width), jnp.bfloat16)], axis=0)
    outgoing = jnp.take(padded, slot_token, axis=0).reshape(experts, capacity, width)
    pieces = outgoing.reshape(devices, quarter, width)
    gathered = lax.all_to_all(pieces, "ep", split_axis=0, concat_axis=0, tiled=True)
    for bit_level in range(levels):
        partner = swapped(gathered, "ep", bit_level)
        upper_bit = position >> bit_level & 1
        first_half = jnp.where(upper_bit == 1, partner, gathered)
        second_half = jnp.where(upper_bit == 1, gathered, partner)
        gathered = jnp.concatenate([first_half, second_half], axis=1)
    partial_value = expert_rows(gathered, gate_weight, up_weight, down_weight)
    length = capacity
    for bit_level in reversed(range(levels)):
        length = length // 2
        upper_bit = position >> bit_level & 1
        kept_rows = lax.dynamic_slice_in_dim(partial_value, upper_bit * length, length, 1)
        sent_rows = lax.dynamic_slice_in_dim(partial_value, (1 - upper_bit) * length, length, 1)
        partial_value = kept_rows + swapped(sent_rows, "ep", bit_level)
    finished = partial_value.astype(jnp.bfloat16)
    returned = lax.all_to_all(finished, "ep", split_axis=0, concat_axis=0, tiled=True)
    results = returned.reshape(experts * capacity, width)
    picked = jnp.take(results, target, axis=0).reshape(tok_rows, top_count, width)
    combined = jnp.sum(route_weight[:, :, None] * picked.astype(jnp.float32), axis=1)
    return combined.astype(jnp.bfloat16)


MESH = pl.DeviceIdType.MESH
HALVES = 2
LANES = 128


def near_plane(z, k, planes):
    below, above = z, planes - 1 - z
    short = jnp.minimum(below, above)
    side = jnp.where(above >= below, 1, -1)
    paired = jnp.where(k % 2 == 1, side * ((k + 1) // 2), -side * (k // 2))
    return z + jnp.where(k <= 2 * short, paired, side * (k - short))


def lane_to_column(row, rows):
    eye = lax.broadcasted_iota(jnp.int32, (rows, rows), 0) == lax.broadcasted_iota(
        jnp.int32, (rows, rows), 1
    )
    return jnp.sum(jnp.where(eye, row, 0.0), axis=1, keepdims=True)


def dense_kernel(
    devices,
    tokens_ref, gain_ref, ids_ref, route_ref, gate_hbm, up_hbm, down_hbm,
    out_ref,
    tok, part, cbuf, ybuf, zbuf, acc, gate, up, down,
    wsem, gsend, grecv, rsend_c, rrecv_c, rsend_y, rrecv_y, rsend_z, rrecv_z,
):
    planes = devices // SPLIT
    rows, width = tokens_ref.shape
    half = rows // HALVES
    me = lax.axis_index("ep")
    z, y, c = me // 4, (me // 2) % 2, me % 2

    def index(zp, yp, cp):
        return zp * 4 + yp * 2 + cp

    ypeer, cpeer = index(z, 1 - y, c), index(z, y, 1 - c)

    def span(h):
        return pl.ds(h * half, half)

    def remote(source, target, send_sem, recv_sem, device):
        return pltpu.make_async_remote_copy(
            src_ref=source, dst_ref=target, send_sem=send_sem, recv_sem=recv_sem,
            device_id={"ep": device}, device_id_type=MESH,
        )

    def move(kind, i, h, device):
        return remote(
            tok.at[i, span(h)], tok.at[i, span(h)], gsend.at[kind, i, h], grecv.at[i, h], device
        )

    weight_loads = [
        pltpu.make_async_copy(gate_hbm.at[0], gate, wsem.at[0]),
        pltpu.make_async_copy(up_hbm.at[0], up, wsem.at[1]),
        pltpu.make_async_copy(down_hbm.at[0], down, wsem.at[2]),
    ]
    for load in weight_loads:
        load.start()

    has_up, has_down = z < planes - 1, z > 0
    barrier = pltpu.get_barrier_semaphore()

    def greet(device):
        pl.semaphore_signal(
            barrier, inc=1, device_id={"ep": device}, device_id_type=MESH
        )

    greet(ypeer)
    greet(cpeer)
    pl.when(has_up)(lambda: greet(me + 4))
    pl.when(has_down)(lambda: greet(me - 4))

    lanes = lax.broadcasted_iota(jnp.int32, (1, LANES), 1)
    routes = jnp.zeros((rows, LANES), jnp.float32)
    for e in range(planes):
        row = jnp.sum(jnp.where(ids_ref[...] == e, route_ref[...], 0.0), axis=0, keepdims=True)
        column = lane_to_column(row, rows)
        high = column.astype(jnp.bfloat16).astype(jnp.float32)
        routes = jnp.where(lanes == e, high, routes)
        routes = jnp.where(lanes == planes + e, column - high, routes)
    tok[me, :, width:] = routes.astype(jnp.bfloat16)
    for h in range(HALVES):
        values = tokens_ref[span(h), :].astype(jnp.float32)
        center = values - jnp.mean(values, axis=-1, keepdims=True)
        spread = jnp.mean(center * center, axis=-1, keepdims=True)
        tok[me, span(h), :width] = (center * lax.rsqrt(spread + EPSILON) * gain_ref[...]).astype(
            jnp.bfloat16
        )
        if h == 0:
            pl.semaphore_wait(
                barrier, 2 + has_up.astype(jnp.int32) + has_down.astype(jnp.int32)
            )
        move(2, me, h, ypeer).start()
        pl.when(has_up)(lambda: move(0, me, h, me + 4).start())
        pl.when(has_down)(lambda: move(1, me, h, me - 4).start())
        move(3, me, h, cpeer).start()
    for load in weight_loads:
        load.wait()

    def onward(zp):
        return jnp.where(zp < z, z + 1, z - 1)

    def exists(plane):
        return jnp.logical_and(plane >= 0, plane < planes)

    def compute(zp, yp):
        first = index(zp, yp, 0)
        x = tok[pl.ds(first, 2), :, :width].reshape(2 * rows, width)
        routes = tok[pl.ds(first, 2), :, width:].reshape(2 * rows, LANES).astype(jnp.float32)
        gate_cut = jnp.minimum(
            jnp.dot(x, gate[...], preferred_element_type=jnp.float32), clamp_limit
        )
        up_cut = jnp.clip(
            jnp.dot(x, up[...], preferred_element_type=jnp.float32), -clamp_limit, clamp_limit
        )
        active = ((up_cut + 1.0) * (gate_cut * jax.nn.sigmoid(gate_cut * sigmoid_slope))).astype(
            jnp.bfloat16
        )
        mine = jnp.logical_or(lanes == z, lanes == planes + z)
        scale = jnp.sum(jnp.where(mine, routes, 0.0), axis=1, keepdims=True)
        tile = min(512, width)
        for start in range(0, width, tile):
            value = jnp.dot(
                active, down[:, start : start + tile], preferred_element_type=jnp.float32
            )
            part[pl.ds(first, 2), :, start : start + tile] = (
                (value * scale).astype(jnp.bfloat16).reshape(2, rows, tile)
            )

    def to_core(zp, yp):
        pair = zp * 2 + yp
        return remote(
            part.at[index(zp, yp, 1 - c)], cbuf.at[pair],
            rsend_c.at[pair], rrecv_c.at[pair], cpeer,
        )

    def beside(plane):
        return jnp.abs(plane - z) == 1

    def pass_up():
        return move(4, index(z, 1 - y, c), 1, me + 4)

    def pass_down():
        return move(5, index(z, 1 - y, c), 1, me - 4)

    def take(i, h):
        move(3, i, h, cpeer).wait_recv()
        move(3, i, h, cpeer).start()

    def group(zp, yp):
        for h in range(HALVES):
            move(3, index(zp, yp, 1 - c), h, cpeer).wait_recv()
        compute(zp, yp)
        to_core(zp, yp).start()

    def gather_step(k, _):
        zk = near_plane(z, jnp.minimum(k, planes - 1), planes)
        zb = near_plane(z, jnp.maximum(k - 1, 0), planes)

        @pl.when(jnp.logical_and(k > 0, k < planes))
        def _():
            i = index(zk, y, c)
            nz = onward(zk)
            for h in range(HALVES):
                move(2, i, h, ypeer).wait_recv()
                pl.when(exists(nz))(lambda: move(0, i, h, index(nz, y, c)).start())
                if h == 0:
                    move(2, i, h, ypeer).start()
                else:
                    pl.when(jnp.logical_not(beside(zk)))(lambda: move(2, i, h, ypeer).start())
                move(3, i, h, cpeer).start()

        @pl.when(k == planes - 1)
        def _():
            inner = jnp.logical_and(has_up, has_down)
            pl.when(inner)(lambda: pass_up().start())
            pl.when(inner)(lambda: pass_down().start())

        @pl.when(k > 0)
        def _():
            i = index(zb, 1 - y, c)
            take(i, 0)
            pl.when(jnp.logical_not(beside(zb)))(lambda: take(i, 1))

        @pl.when(k == 1)
        def _():
            pl.when(jnp.logical_not(has_down))(lambda: pass_up().start())
            pl.when(jnp.logical_not(has_up))(lambda: pass_down().start())

        def group_step(j, _):
            zp = jnp.where(j == 0, zk, zb)
            yp = jnp.where(j == 0, y, 1 - y)
            ready = jnp.where(beside(zb), 0, k)
            pl.when(jnp.where(j == 0, planes - k, ready) > 0)(lambda: group(zp, yp))
            return 0

        lax.fori_loop(0, 2, group_step, 0)
        return 0

    lax.fori_loop(0, planes + 1, gather_step, 0)

    def to_y(zp, h):
        return remote(
            part.at[index(zp, 1 - y, c), span(h)], ybuf.at[zp, span(h)],
            rsend_y.at[zp, h], rrecv_y.at[zp, h], ypeer,
        )

    def from_y(zp, h):
        return remote(
            part.at[index(zp, y, c), span(h)], ybuf.at[zp, span(h)],
            rsend_y.at[zp, h], rrecv_y.at[zp, h], ypeer,
        )

    def spread_step(t, _):
        zp = near_plane(z, planes - 1 - t, planes)
        i = index(zp, 1 - y, c)

        @pl.when(beside(zp))
        def _():
            take(i, 1)
            group(zp, 1 - y)

        to_core(zp, 1 - y).wait_recv()
        for h in range(HALVES):
            part[i, span(h), :] = (
                part[i, span(h), :].astype(jnp.float32)
                + cbuf[zp * 2 + 1 - y, span(h), :].astype(jnp.float32)
            ).astype(jnp.bfloat16)
            to_y(zp, h).start()
        return 0

    lax.fori_loop(0, planes, spread_step, 0)

    def hop(zp, h):
        nz = jnp.where(zp > z, z + 1, z - 1)
        slot = jnp.where(jnp.logical_and(nz == zp, zp < z), planes, zp)
        return remote(
            part.at[index(zp, y, c), span(h)], zbuf.at[slot, span(h)],
            rsend_z.at[zp, h], rrecv_z.at[slot, h], index(nz, y, c),
        )

    def landed(slot, h):
        return remote(
            part.at[me, span(h)], zbuf.at[slot, span(h)],
            rsend_z.at[z, h], rrecv_z.at[slot, h], ypeer,
        )

    def add_landed(slot, h):
        landed(slot, h).wait_recv()
        acc[...] += zbuf[slot, span(h), :].astype(jnp.float32)

    def total(zp, h):
        from_y(zp, h).wait_recv()
        acc[...] = (
            part[index(zp, y, c), span(h), :].astype(jnp.float32)
            + cbuf[zp * 2 + y, span(h), :].astype(jnp.float32)
            + ybuf[zp, span(h), :].astype(jnp.float32)
        )

    def chain_step(t, _):
        zp = near_plane(z, planes - 1 - t, planes)
        to_core(zp, y).wait_recv()
        for h in range(HALVES):
            total(zp, h)
            pl.when(jnp.where(zp > z, has_down, has_up))(lambda: add_landed(zp, h))
            part[index(zp, y, c), span(h), :] = acc[...].astype(jnp.bfloat16)
            hop(zp, h).start()
        return 0

    lax.fori_loop(0, planes - 1, chain_step, 0)
    to_core(z, y).wait_recv()
    for h in range(HALVES):
        total(z, h)
        pl.when(has_down)(lambda: add_landed(z, h))
        pl.when(has_up)(lambda: add_landed(planes, h))
        out_ref[span(h), :] = acc[...].astype(jnp.bfloat16)

    for h in range(HALVES):
        move(2, me, h, ypeer).wait_send()
        pl.when(has_up)(lambda: move(0, me, h, me + 4).wait_send())
        pl.when(has_down)(lambda: move(1, me, h, me - 4).wait_send())
        move(3, me, h, cpeer).wait_send()

    pl.when(has_up)(lambda: pass_up().wait_send())
    pl.when(has_down)(lambda: pass_down().wait_send())

    def drain_step(k, _):
        zp = near_plane(z, k, planes)
        to_core(zp, y).wait_send()
        to_core(zp, 1 - y).wait_send()
        for h in range(HALVES):
            move(3, index(zp, 1 - y, c), h, cpeer).wait_send()
            to_y(zp, h).wait_send()

        @pl.when(k > 0)
        def _():
            i = index(zp, y, c)
            nz = onward(zp)
            for h in range(HALVES):
                pl.when(exists(nz))(lambda: move(0, i, h, index(nz, y, c)).wait_send())
                if h == 0:
                    move(2, i, h, ypeer).wait_send()
                else:
                    pl.when(jnp.logical_not(beside(zp)))(
                        lambda: move(2, i, h, ypeer).wait_send()
                    )
                move(3, i, h, cpeer).wait_send()
                hop(zp, h).wait_send()

        return 0

    lax.fori_loop(0, planes, drain_step, 0)


def dense_body(tokens, norm_gain, expert_ids, route_weight, gate_weight, up_weight, down_weight):
    devices = lax.axis_size("ep")
    planes = devices // SPLIT
    rows, width = tokens.shape
    hidden = gate_weight.shape[2]
    half = rows // HALVES
    vmem, dma = pltpu.VMEM, pltpu.SemaphoreType.DMA
    block = jnp.bfloat16
    return pl.pallas_call(
        functools.partial(dense_kernel, devices),
        out_shape=jax.ShapeDtypeStruct((rows, width), block),
        in_specs=[pl.BlockSpec(memory_space=vmem)] * 4 + [pl.BlockSpec(memory_space=pl.ANY)] * 3,
        out_specs=pl.BlockSpec(memory_space=vmem),
        scratch_shapes=[
            vmem((devices, rows, width + LANES), block),
            vmem((devices, rows, width), block),
            vmem((2 * planes, rows, width), block),
            vmem((planes, rows, width), block),
            vmem((planes + 1, rows, width), block),
            vmem((half, width), jnp.float32),
            vmem((width, hidden), block),
            vmem((width, hidden), block),
            vmem((hidden, width), block),
            dma((3,)),
            dma((6, devices, HALVES)),
            dma((devices, HALVES)),
            dma((2 * planes,)),
            dma((2 * planes,)),
            dma((planes, HALVES)),
            dma((planes, HALVES)),
            dma((planes, HALVES)),
            dma((planes + 1, HALVES)),
        ],
        compiler_params=pltpu.CompilerParams(
            collective_id=0, has_side_effects=True, vmem_limit_bytes=60 * 1024 * 1024
        ),
        name="dense_experts",
    )(
        tokens, norm_gain.reshape(1, width), expert_ids.T, route_weight.T,
        gate_weight, up_weight, down_weight,
    )


def body(tokens, norm_gain, expert_ids, route_weight, gate_weight, up_weight, down_weight):
    tok_rows, top_count = expert_ids.shape
    experts = lax.axis_size("ep") // SPLIT
    capacity = min(tok_rows, 2 * tok_rows * top_count // experts)
    chosen = dense_body if capacity == tok_rows else slot_body
    return chosen(
        tokens, norm_gain, expert_ids, route_weight, gate_weight, up_weight, down_weight
    )


def solution(mesh):
    placed = (
        P(("grp", "ep"), None),
        P(),
        P(("grp", "ep"), None),
        P(("grp", "ep"), None),
        P("ep", None, None),
        P("ep", None, None),
        P("ep", None, None),
    )
    return jax.shard_map(
        body, mesh=mesh, in_specs=placed, out_specs=P(("grp", "ep"), None), check_vma=False
    )
```

```python
import functools

import jax
import jax.numpy as jnp
from jax import lax
from jax.experimental import pallas as pl
from jax.experimental.pallas import tpu as pltpu
from jax.sharding import PartitionSpec as P

SPLIT = 4


EPSILON = 1e-05
clamp_limit = 7.0
sigmoid_slope = 1.702


def swapped(array, axis, bit):
    return lax.ppermute(array, axis, [(i, i ^ 1 << bit) for i in range(lax.axis_size(axis))])


def layer_norm(tokens, norm_gain):
    values = tokens.astype(jnp.float32)
    center = values - jnp.mean(values, axis=-1, keepdims=True)
    spread = jnp.mean(center * center, axis=-1, keepdims=True)
    return (center * lax.rsqrt(spread + EPSILON) * norm_gain).astype(jnp.bfloat16)


def expert_rows(block_rows, gate_weight, up_weight, down_weight):
    gate_pre = jnp.einsum(
        "scd,df->scf", block_rows, gate_weight[0], preferred_element_type=jnp.float32
    )
    up_pre = jnp.einsum("scd,df->scf", block_rows, up_weight[0], preferred_element_type=jnp.float32)
    gate_cut = jnp.minimum(gate_pre, clamp_limit)
    up_cut = jnp.clip(up_pre, -clamp_limit, clamp_limit)
    active = ((up_cut + 1.0) * (gate_cut * jax.nn.sigmoid(gate_cut * sigmoid_slope))).astype(
        jnp.bfloat16
    )
    return jnp.einsum("scf,fd->scd", active, down_weight[0], preferred_element_type=jnp.float32)


def slot_body(tokens, norm_gain, expert_ids, route_weight, gate_weight, up_weight, down_weight):
    normed = layer_norm(tokens, norm_gain)
    devices = lax.axis_size("ep")
    experts = devices // SPLIT
    tok_rows = tokens.shape[0]
    top_count = expert_ids.shape[1]
    width = tokens.shape[1]
    capacity = min(tok_rows, 2 * tok_rows * top_count // experts)
    quarter = capacity // SPLIT
    levels = SPLIT.bit_length() - 1
    position = lax.axis_index("ep")
    flat_ids = expert_ids.reshape(-1)
    onehot = (flat_ids[:, None] == jnp.arange(experts, dtype=jnp.int32)[None, :]).astype(jnp.int32)
    earlier = jnp.cumsum(onehot, axis=0) - onehot
    slot_index = jnp.sum(earlier * onehot, axis=1)
    target = flat_ids * capacity + slot_index
    owners = jnp.arange(flat_ids.shape[0], dtype=jnp.int32) // top_count
    slot_token = jnp.full((experts * capacity,), tok_rows, jnp.int32).at[target].set(owners)
    padded = jnp.concatenate([normed, jnp.zeros((1, width), jnp.bfloat16)], axis=0)
    outgoing = jnp.take(padded, slot_token, axis=0).reshape(experts, capacity, width)
    pieces = outgoing.reshape(devices, quarter, width)
    gathered = lax.all_to_all(pieces, "ep", split_axis=0, concat_axis=0, tiled=True)
    for bit_level in range(levels):
        partner = swapped(gathered, "ep", bit_level)
        upper_bit = position >> bit_level & 1
        first_half = jnp.where(upper_bit == 1, partner, gathered)
        second_half = jnp.where(upper_bit == 1, gathered, partner)
        gathered = jnp.concatenate([first_half, second_half], axis=1)
    partial_value = expert_rows(gathered, gate_weight, up_weight, down_weight)
    length = capacity
    for bit_level in reversed(range(levels)):
        length = length // 2
        upper_bit = position >> bit_level & 1
        kept_rows = lax.dynamic_slice_in_dim(partial_value, upper_bit * length, length, 1)
        sent_rows = lax.dynamic_slice_in_dim(partial_value, (1 - upper_bit) * length, length, 1)
        partial_value = kept_rows + swapped(sent_rows, "ep", bit_level)
    finished = partial_value.astype(jnp.bfloat16)
    returned = lax.all_to_all(finished, "ep", split_axis=0, concat_axis=0, tiled=True)
    results = returned.reshape(experts * capacity, width)
    picked = jnp.take(results, target, axis=0).reshape(tok_rows, top_count, width)
    combined = jnp.sum(route_weight[:, :, None] * picked.astype(jnp.float32), axis=1)
    return combined.astype(jnp.bfloat16)


MESH = pl.DeviceIdType.MESH
HALVES = 2
LANES = 128


def near_plane(z, k, planes):
    below, above = z, planes - 1 - z
    short = jnp.minimum(below, above)
    side = jnp.where(above >= below, 1, -1)
    paired = jnp.where(k % 2 == 1, side * ((k + 1) // 2), -side * (k // 2))
    return z + jnp.where(k <= 2 * short, paired, side * (k - short))


def lane_to_column(row, rows):
    eye = lax.broadcasted_iota(jnp.int32, (rows, rows), 0) == lax.broadcasted_iota(
        jnp.int32, (rows, rows), 1
    )
    return jnp.sum(jnp.where(eye, row, 0.0), axis=1, keepdims=True)


def dense_kernel(
    devices,
    tokens_ref, gain_ref, ids_ref, route_ref, gate_hbm, up_hbm, down_hbm,
    out_ref,
    tok, part, cbuf, ybuf, zbuf, acc, gate, up, down,
    wsem, gsend, grecv, rsend_c, rrecv_c, rsend_y, rrecv_y, rsend_z, rrecv_z,
):
    planes = devices // SPLIT
    rows, width = tokens_ref.shape
    half = rows // HALVES
    me = lax.axis_index("ep")
    z, y, c = me // 4, (me // 2) % 2, me % 2

    def index(zp, yp, cp):
        return zp * 4 + yp * 2 + cp

    ypeer, cpeer = index(z, 1 - y, c), index(z, y, 1 - c)

    def span(h):
        return pl.ds(h * half, half)

    def remote(source, target, send_sem, recv_sem, device):
        return pltpu.make_async_remote_copy(
            src_ref=source, dst_ref=target, send_sem=send_sem, recv_sem=recv_sem,
            device_id={"ep": device}, device_id_type=MESH,
        )

    def move(kind, i, h, device):
        return remote(
            tok.at[i, span(h)], tok.at[i, span(h)], gsend.at[kind, i, h], grecv.at[i, h], device
        )

    weight_loads = [
        pltpu.make_async_copy(gate_hbm.at[0], gate, wsem.at[0]),
        pltpu.make_async_copy(up_hbm.at[0], up, wsem.at[1]),
        pltpu.make_async_copy(down_hbm.at[0], down, wsem.at[2]),
    ]
    for load in weight_loads:
        load.start()

    has_up, has_down = z < planes - 1, z > 0
    barrier = pltpu.get_barrier_semaphore()

    def greet(device):
        pl.semaphore_signal(
            barrier, inc=1, device_id={"ep": device}, device_id_type=MESH
        )

    greet(ypeer)
    greet(cpeer)
    pl.when(has_up)(lambda: greet(me + 4))
    pl.when(has_down)(lambda: greet(me - 4))

    lanes = lax.broadcasted_iota(jnp.int32, (1, LANES), 1)
    routes = jnp.zeros((rows, LANES), jnp.float32)
    for e in range(planes):
        row = jnp.sum(jnp.where(ids_ref[...] == e, route_ref[...], 0.0), axis=0, keepdims=True)
        column = lane_to_column(row, rows)
        high = column.astype(jnp.bfloat16).astype(jnp.float32)
        routes = jnp.where(lanes == e, high, routes)
        routes = jnp.where(lanes == planes + e, column - high, routes)
    tok[me, :, width:] = routes.astype(jnp.bfloat16)
    for h in range(HALVES):
        values = tokens_ref[span(h), :].astype(jnp.float32)
        center = values - jnp.mean(values, axis=-1, keepdims=True)
        spread = jnp.mean(center * center, axis=-1, keepdims=True)
        tok[me, span(h), :width] = (center * lax.rsqrt(spread + EPSILON) * gain_ref[...]).astype(
            jnp.bfloat16
        )
        if h == 0:
            pl.semaphore_wait(
                barrier, 2 + has_up.astype(jnp.int32) + has_down.astype(jnp.int32)
            )
        move(2, me, h, ypeer).start()
        pl.when(has_up)(lambda: move(0, me, h, me + 4).start())
        pl.when(has_down)(lambda: move(1, me, h, me - 4).start())
        move(3, me, h, cpeer).start()
    for load in weight_loads:
        load.wait()

    def onward(zp):
        return jnp.where(zp < z, z + 1, z - 1)

    def exists(plane):
        return jnp.logical_and(plane >= 0, plane < planes)

    def compute(zp, yp):
        first = index(zp, yp, 0)
        x = tok[pl.ds(first, 2), :, :width].reshape(2 * rows, width)
        routes = tok[pl.ds(first, 2), :, width:].reshape(2 * rows, LANES).astype(jnp.float32)
        gate_cut = jnp.minimum(
            jnp.dot(x, gate[...], preferred_element_type=jnp.float32), clamp_limit
        )
        up_cut = jnp.clip(
            jnp.dot(x, up[...], preferred_element_type=jnp.float32), -clamp_limit, clamp_limit
        )
        active = ((up_cut + 1.0) * (gate_cut * jax.nn.sigmoid(gate_cut * sigmoid_slope))).astype(
            jnp.bfloat16
        )
        mine = jnp.logical_or(lanes == z, lanes == planes + z)
        scale = jnp.sum(jnp.where(mine, routes, 0.0), axis=1, keepdims=True)
        tile = min(512, width)
        for start in range(0, width, tile):
            value = jnp.dot(
                active, down[:, start : start + tile], preferred_element_type=jnp.float32
            )
            part[pl.ds(first, 2), :, start : start + tile] = (
                (value * scale).astype(jnp.bfloat16).reshape(2, rows, tile)
            )

    def to_core(zp, yp):
        pair = zp * 2 + yp
        return remote(
            part.at[index(zp, yp, 1 - c)], cbuf.at[pair],
            rsend_c.at[pair], rrecv_c.at[pair], cpeer,
        )

    def beside(plane):
        return jnp.abs(plane - z) == 1

    def pass_up():
        return move(4, index(z, 1 - y, c), 1, me + 4)

    def pass_down():
        return move(5, index(z, 1 - y, c), 1, me - 4)

    def take(i, h):
        move(3, i, h, cpeer).wait_recv()
        move(3, i, h, cpeer).start()

    def group(zp, yp):
        for h in range(HALVES):
            move(3, index(zp, yp, 1 - c), h, cpeer).wait_recv()
        compute(zp, yp)
        to_core(zp, yp).start()

    def to_y(zp, h):
        return remote(
            part.at[index(zp, 1 - y, c), span(h)], ybuf.at[zp, span(h)],
            rsend_y.at[zp, h], rrecv_y.at[zp, h], ypeer,
        )

    def spread_half(zp, h):
        i = index(zp, 1 - y, c)
        part[i, span(h), :] = (
            part[i, span(h), :].astype(jnp.float32)
            + cbuf[zp * 2 + 1 - y, span(h), :].astype(jnp.float32)
        ).astype(jnp.bfloat16)
        to_y(zp, h).start()

    def gather_step(k, _):
        zk = near_plane(z, jnp.minimum(k, planes - 1), planes)
        zb = near_plane(z, jnp.maximum(k - 1, 0), planes)

        @pl.when(k == planes)
        def _():
            to_core(z, 1 - y).wait_recv()
            spread_half(z, 0)

        @pl.when(jnp.logical_and(k > 0, k < planes))
        def _():
            i = index(zk, y, c)
            nz = onward(zk)
            for h in range(HALVES):
                move(2, i, h, ypeer).wait_recv()
                pl.when(exists(nz))(lambda: move(0, i, h, index(nz, y, c)).start())
                if h == 0:
                    move(2, i, h, ypeer).start()
                else:
                    pl.when(jnp.logical_not(beside(zk)))(lambda: move(2, i, h, ypeer).start())
                move(3, i, h, cpeer).start()

        @pl.when(k == planes - 1)
        def _():
            inner = jnp.logical_and(has_up, has_down)
            pl.when(inner)(lambda: pass_up().start())
            pl.when(inner)(lambda: pass_down().start())

        @pl.when(k > 0)
        def _():
            i = index(zb, 1 - y, c)
            take(i, 0)
            pl.when(jnp.logical_not(beside(zb)))(lambda: take(i, 1))

        @pl.when(k == 1)
        def _():
            pl.when(jnp.logical_not(has_down))(lambda: pass_up().start())
            pl.when(jnp.logical_not(has_up))(lambda: pass_down().start())

        def group_step(j, _):
            zp = jnp.where(j == 0, zk, zb)
            yp = jnp.where(j == 0, y, 1 - y)
            ready = jnp.where(beside(zb), 0, k)
            pl.when(jnp.where(j == 0, planes - k, ready) > 0)(lambda: group(zp, yp))
            return 0

        lax.fori_loop(0, 2, group_step, 0)
        return 0

    lax.fori_loop(0, planes + 1, gather_step, 0)

    def from_y(zp, h):
        return remote(
            part.at[index(zp, y, c), span(h)], ybuf.at[zp, span(h)],
            rsend_y.at[zp, h], rrecv_y.at[zp, h], ypeer,
        )

    def spread_step(t, _):
        zp = near_plane(z, planes - 1 - t, planes)
        i = index(zp, 1 - y, c)

        @pl.when(beside(zp))
        def _():
            take(i, 1)
            group(zp, 1 - y)

        @pl.when(zp != z)
        def _():
            to_core(zp, 1 - y).wait_recv()
            spread_half(zp, 0)

        spread_half(zp, 1)
        return 0

    lax.fori_loop(0, planes, spread_step, 0)

    def hop(zp, h):
        nz = jnp.where(zp > z, z + 1, z - 1)
        slot = jnp.where(jnp.logical_and(nz == zp, zp < z), planes, zp)
        return remote(
            part.at[index(zp, y, c), span(h)], zbuf.at[slot, span(h)],
            rsend_z.at[zp, h], rrecv_z.at[slot, h], index(nz, y, c),
        )

    def landed(slot, h):
        return remote(
            part.at[me, span(h)], zbuf.at[slot, span(h)],
            rsend_z.at[z, h], rrecv_z.at[slot, h], ypeer,
        )

    def add_landed(slot, h):
        landed(slot, h).wait_recv()
        acc[...] += zbuf[slot, span(h), :].astype(jnp.float32)

    def total(zp, h):
        from_y(zp, h).wait_recv()
        acc[...] = (
            part[index(zp, y, c), span(h), :].astype(jnp.float32)
            + cbuf[zp * 2 + y, span(h), :].astype(jnp.float32)
            + ybuf[zp, span(h), :].astype(jnp.float32)
        )

    def chain_step(t, _):
        zp = near_plane(z, planes - 1 - t, planes)
        to_core(zp, y).wait_recv()
        for h in range(HALVES):
            total(zp, h)
            pl.when(jnp.where(zp > z, has_down, has_up))(lambda: add_landed(zp, h))
            part[index(zp, y, c), span(h), :] = acc[...].astype(jnp.bfloat16)
            hop(zp, h).start()
        return 0

    lax.fori_loop(0, planes - 1, chain_step, 0)
    to_core(z, y).wait_recv()
    for h in range(HALVES):
        total(z, h)
        pl.when(has_down)(lambda: add_landed(z, h))
        pl.when(has_up)(lambda: add_landed(planes, h))
        out_ref[span(h), :] = acc[...].astype(jnp.bfloat16)

    for h in range(HALVES):
        move(2, me, h, ypeer).wait_send()
        pl.when(has_up)(lambda: move(0, me, h, me + 4).wait_send())
        pl.when(has_down)(lambda: move(1, me, h, me - 4).wait_send())
        move(3, me, h, cpeer).wait_send()

    pl.when(has_up)(lambda: pass_up().wait_send())
    pl.when(has_down)(lambda: pass_down().wait_send())

    def drain_step(k, _):
        zp = near_plane(z, k, planes)
        to_core(zp, y).wait_send()
        to_core(zp, 1 - y).wait_send()
        for h in range(HALVES):
            move(3, index(zp, 1 - y, c), h, cpeer).wait_send()
            to_y(zp, h).wait_send()

        @pl.when(k > 0)
        def _():
            i = index(zp, y, c)
            nz = onward(zp)
            for h in range(HALVES):
                pl.when(exists(nz))(lambda: move(0, i, h, index(nz, y, c)).wait_send())
                if h == 0:
                    move(2, i, h, ypeer).wait_send()
                else:
                    pl.when(jnp.logical_not(beside(zp)))(
                        lambda: move(2, i, h, ypeer).wait_send()
                    )
                move(3, i, h, cpeer).wait_send()
                hop(zp, h).wait_send()

        return 0

    lax.fori_loop(0, planes, drain_step, 0)


def dense_body(tokens, norm_gain, expert_ids, route_weight, gate_weight, up_weight, down_weight):
    devices = lax.axis_size("ep")
    planes = devices // SPLIT
    rows, width = tokens.shape
    hidden = gate_weight.shape[2]
    half = rows // HALVES
    vmem, dma = pltpu.VMEM, pltpu.SemaphoreType.DMA
    block = jnp.bfloat16
    return pl.pallas_call(
        functools.partial(dense_kernel, devices),
        out_shape=jax.ShapeDtypeStruct((rows, width), block),
        in_specs=[pl.BlockSpec(memory_space=vmem)] * 4 + [pl.BlockSpec(memory_space=pl.ANY)] * 3,
        out_specs=pl.BlockSpec(memory_space=vmem),
        scratch_shapes=[
            vmem((devices, rows, width + LANES), block),
            vmem((devices, rows, width), block),
            vmem((2 * planes, rows, width), block),
            vmem((planes, rows, width), block),
            vmem((planes + 1, rows, width), block),
            vmem((half, width), jnp.float32),
            vmem((width, hidden), block),
            vmem((width, hidden), block),
            vmem((hidden, width), block),
            dma((3,)),
            dma((6, devices, HALVES)),
            dma((devices, HALVES)),
            dma((2 * planes,)),
            dma((2 * planes,)),
            dma((planes, HALVES)),
            dma((planes, HALVES)),
            dma((planes, HALVES)),
            dma((planes + 1, HALVES)),
        ],
        compiler_params=pltpu.CompilerParams(
            collective_id=0, has_side_effects=True, vmem_limit_bytes=60 * 1024 * 1024
        ),
        name="dense_experts",
    )(
        tokens, norm_gain.reshape(1, width), expert_ids.T, route_weight.T,
        gate_weight, up_weight, down_weight,
    )


def body(tokens, norm_gain, expert_ids, route_weight, gate_weight, up_weight, down_weight):
    tok_rows, top_count = expert_ids.shape
    experts = lax.axis_size("ep") // SPLIT
    capacity = min(tok_rows, 2 * tok_rows * top_count // experts)
    chosen = dense_body if capacity == tok_rows else slot_body
    return chosen(
        tokens, norm_gain, expert_ids, route_weight, gate_weight, up_weight, down_weight
    )


def solution(mesh):
    placed = (
        P(("grp", "ep"), None),
        P(),
        P(("grp", "ep"), None),
        P(("grp", "ep"), None),
        P("ep", None, None),
        P("ep", None, None),
        P("ep", None, None),
    )
    return jax.shard_map(
        body, mesh=mesh, in_specs=placed, out_specs=P(("grp", "ep"), None), check_vma=False
    )
```
